32 devices in a mesh: sp: 16 (over z, y, core), tp: 2 (over x).
Axes of the slice: x: 2, y: 2, z: 4, core: 2. Of those that a mesh axis runs over, the one named last changes fastest.
Arguments:
- asking_matrix: bfloat16 [2048, 2048], P('sp', 'tp'), may hold values from -30 to 30
- matching_key_matrix: bfloat16 [2048, 1024], P('sp', 'tp'), may hold values from -30 to 30
- carried_value_matrix: bfloat16 [2048, 1024], P('sp', 'tp'), may hold values from -48 to 48
- silu_switch_argument: bfloat16 [2048, 2048], P('sp', 'tp'), may hold values from -6 to 6
- duality_source_matrix: bfloat16 [2048, 2048], P('sp', 'tp'), may hold values from -6 to 6
- storing_direction_matrix: bfloat16 [2048, 1024], P('sp', 'tp'), may hold values from -6 to 6
- fetching_direction_matrix: bfloat16 [2048, 1024], P('sp', 'tp'), may hold values from -6 to 6
- duality_kernel_coefficients: bfloat16 [5, 2048], P(None, 'tp'), may hold values from -2.5 to 2.5
- storing_kernel_coefficients: bfloat16 [5, 1024], P(None, 'tp'), may hold values from -2.5 to 2.5
- fetching_kernel_coefficients: bfloat16 [5, 1024], P(None, 'tp'), may hold values from -2.5 to 2.5
- raw_increment_lengths: float32 [2, 32, 2048], P(None, 'tp', 'sp'), may hold values from -5.5 to 5.5
- logarithmic_fading_speeds: float32 [2, 32], P(None, 'tp'), may hold values from -16 to -2.9
- token_fading_spikes: float32 [2, 32, 2048], P(None, 'tp', 'sp'), may hold values from -2.1 to 0
- absorber_score_vector: float32 [16], P('tp'), may hold values from 4 to 8
- cluster_scaling_factor: float32 [2048], P('tp'), may hold values from 0.1 to 1.9
- final_mapping_matrix: bfloat16 [2, 2048, 4096], P(None, 'tp', 'sp'), may hold values from -0.09375 to 0.09375
Outputs:
- mixed_out: bfloat16 [2048, 4096], P(('sp', 'tp'))
The draws below stay inside these ranges and needn't reach their ends.
All inputs are finite; a program needn't handle non-finite values.
Results may differ from the reference program's by a relative error of at most 0.014.
Values may be sent and summed in bfloat16 or wider, within the bound.
A program may use at most 128 MiB of HBM per device.

```python
import math
import jax
import jax.numpy as jnp
from jax import lax

D = 4096
HEADS = 16
KV_HEADS = 8
HEAD = 128
SSD_HEADS = 32
SSD_HEAD = 64
GROUPS = 8
STATE = 128
CONV = 5
WINDOW = 128
SPAN = 128
TOK_DEV = 128
TOKENS = 2048
ATTN_W = 2048
KV_W = 1024
SSD_W = 2048
N_TP = 2


def drawn_rows(key):
    query_base = jnp.clip(jax.random.normal(jax.random.fold_in(key, 11), (TOKENS, ATTN_W), jnp.float32), -4.0, 4.0)
    key_base = jnp.clip(jax.random.normal(jax.random.fold_in(key, 12), (TOKENS, KV_W), jnp.float32), -4.0, 4.0)
    return (query_base, key_base)


def draw_asking_matrix(key, part):
    return drawn_rows(key)[0].astype(jnp.bfloat16)


def draw_matching_key_matrix(key, part):
    return drawn_rows(key)[1].astype(jnp.bfloat16)


def draw_raw_increment_lengths(key, part):
    jitter = jnp.clip(jax.random.normal(jax.random.fold_in(key, 21), (2, SSD_HEADS, TOKENS), jnp.float32), -4.0, 4.0)
    block_level = jax.random.uniform(jax.random.fold_in(key, 22), (2, SSD_HEADS, TOKENS // TOK_DEV), jnp.float32, -1.5, 1.5)
    return jitter + jnp.repeat(block_level, TOK_DEV, axis=2)


def draw_logarithmic_fading_speeds(key, part):
    keep_count = SSD_HEADS // 2
    ranking = jnp.stack([jax.random.permutation(jax.random.fold_in(key, 31), SSD_HEADS), jax.random.permutation(jax.random.fold_in(key, 32), SSD_HEADS)])
    lasting = ranking < keep_count
    slow_rate = jnp.exp(jax.random.uniform(jax.random.fold_in(key, 33), (2, SSD_HEADS), jnp.float32, math.log(0.02), math.log(0.3))) / TOKENS
    fast_rate = jnp.exp(jax.random.uniform(jax.random.fold_in(key, 34), (2, SSD_HEADS), jnp.float32, math.log(1.0 / 70.0), math.log(1.0 / 20.0)))
    return jnp.log(jnp.where(lasting, slow_rate, fast_rate))


def draw_token_fading_spikes(key, part):
    positions = jax.random.randint(jax.random.fold_in(key, 41), (2, SSD_HEADS, 3), 0, TOKENS)
    depths = jax.random.uniform(jax.random.fold_in(key, 42), (2, SSD_HEADS, 3), jnp.float32, 0.22, 0.69)
    places = jnp.arange(TOKENS, dtype=jnp.int32)
    hits = jnp.where(places[None, None, None, :] == positions[..., None], depths[..., None], 0.0)
    return -jnp.sum(hits, axis=2)


def block_levels(rng, dims, shards, smallest, top_value):
    loudness, own = 1.0, jax.random.fold_in(rng, 6)
    for position, blocks in shards:
        heights = jnp.exp(jax.random.uniform(jax.random.fold_in(own, position), (blocks,), jnp.float32, smallest / len(shards), top_value / len(shards)))
        loudness = loudness * jnp.repeat(heights, dims[position] // blocks).reshape([-1 if axis == position else 1 for axis in range(len(dims))])
    return loudness


def noise(stream_key, shape, scale, most, split=(), held_as=jnp.bfloat16):
    gain = block_levels(stream_key, shape, split, -0.22, 0.18) if split else 1.0
    values = jax.random.normal(stream_key, shape, jnp.float32) * scale * gain
    return jnp.minimum(jnp.maximum(values, -most), most).astype(held_as)


def setup_inputs(seed: int = 0) -> dict:
    key_of = jax.random.split(jax.random.key(seed), 17)
    asking_matrix = draw_asking_matrix(jax.random.fold_in(key_of[16], 71), 0)
    matching_key_matrix = draw_matching_key_matrix(jax.random.fold_in(key_of[16], 71), 0)
    carried_value_matrix = noise(key_of[2], (TOKENS, KV_W), 8.0, 48.0, ((0, 16), (1, 2)))
    silu_switch_argument = noise(key_of[3], (TOKENS, SSD_W), 1.0, 6.0, ((0, 16), (1, 2)))
    duality_source_matrix = noise(key_of[4], (TOKENS, SSD_W), 1.0, 6.0, ((0, 16), (1, 2)))
    storing_direction_matrix = noise(key_of[5], (TOKENS, GROUPS * STATE), 1.0, 6.0, ((0, 16), (1, 2)))
    fetching_direction_matrix = noise(key_of[6], (TOKENS, GROUPS * STATE), 1.0, 6.0, ((0, 16), (1, 2)))
    duality_kernel_coefficients = noise(key_of[7], (CONV, SSD_W), CONV ** -0.5, 2.5, ((1, 2),))
    storing_kernel_coefficients = noise(key_of[8], (CONV, GROUPS * STATE), CONV ** -0.5, 2.5, ((1, 2),))
    fetching_kernel_coefficients = noise(key_of[9], (CONV, GROUPS * STATE), CONV ** -0.5, 2.5, ((1, 2),))
    raw_increment_lengths = draw_raw_increment_lengths(jax.random.fold_in(key_of[16], 71), 0)
    logarithmic_fading_speeds = draw_logarithmic_fading_speeds(jax.random.fold_in(key_of[16], 71), 0)
    token_fading_spikes = draw_token_fading_spikes(jax.random.fold_in(key_of[16], 71), 0)
    absorber_score_vector = jnp.clip(4.0 + 4.0 * jax.random.uniform(key_of[13], (HEADS,), jnp.float32) ** block_levels(key_of[13], (HEADS,), ((0, 2),), -0.2, 0.2), 4.0, 8.0)
    cluster_scaling_factor = jnp.clip(1.0 + 0.18 * jax.random.normal(key_of[14], (SSD_W,), jnp.float32), 0.1, 1.9)
    final_mapping_matrix = noise(key_of[15], (2, ATTN_W, D), (2 * ATTN_W) ** -0.5, 0.09375, ((1, 2), (2, 16)))
    return {"asking_matrix": asking_matrix, "matching_key_matrix": matching_key_matrix, "carried_value_matrix": carried_value_matrix, "silu_switch_argument": silu_switch_argument, "duality_source_matrix": duality_source_matrix, "storing_direction_matrix": storing_direction_matrix, "fetching_direction_matrix": fetching_direction_matrix, "duality_kernel_coefficients": duality_kernel_coefficients, "storing_kernel_coefficients": storing_kernel_coefficients, "fetching_kernel_coefficients": fetching_kernel_coefficients, "raw_increment_lengths": raw_increment_lengths, "logarithmic_fading_speeds": logarithmic_fading_speeds, "token_fading_spikes": token_fading_spikes, "absorber_score_vector": absorber_score_vector, "cluster_scaling_factor": cluster_scaling_factor, "final_mapping_matrix": final_mapping_matrix}


ROTARY_BASE = 500000.0
EPSILON = 1e-06

def rotate(matrix, offset):
    row_count = matrix.shape[0]
    halfway = HEAD // 2
    heads_here = matrix.shape[1] // HEAD
    spacing = ROTARY_BASE ** (-jnp.arange(halfway, dtype=jnp.float32) * 2.0 / HEAD)
    places = (offset + jnp.arange(row_count, dtype=jnp.int32)).astype(jnp.float32)
    angles = places[:, None] * spacing[None, :]
    cosine = jnp.cos(angles)[:, None, :]
    sine_table = jnp.sin(angles)[:, None, :]
    halves = matrix.astype(jnp.float32).reshape(row_count, heads_here, 2, halfway)
    former = halves[:, :, 0]
    latter = halves[:, :, 1]
    turned = jnp.stack([former * cosine - latter * sine_table, latter * cosine + former * sine_table], axis=2)
    return turned.reshape(row_count, heads_here * HEAD).astype(jnp.bfloat16)

def attend(turned_queries, turned_keys, carried_value_matrix, absorber_score_vector):
    sharing = HEADS // KV_HEADS
    block_count = TOKENS // SPAN
    filler = jnp.zeros((SPAN, KV_W), jnp.bfloat16)
    key_pad = jnp.concatenate([filler, turned_keys, filler], axis=0)
    value_pad = jnp.concatenate([filler, carried_value_matrix, filler], axis=0)
    within = jnp.arange(SPAN, dtype=jnp.int32)[:, None]
    across = jnp.arange(3 * SPAN, dtype=jnp.int32)[None, :]
    inside = jnp.abs(across - SPAN - within) <= WINDOW
    sink_rows = absorber_score_vector.reshape(KV_HEADS, sharing)[:, :, None, None]

    def one_block(block_index):
        first_row = (block_index * SPAN).astype(jnp.int32)
        query_tile = lax.dynamic_slice_in_dim(turned_queries, first_row, SPAN, 0).reshape(SPAN, KV_HEADS, sharing, HEAD)
        key_tile = lax.dynamic_slice_in_dim(key_pad, first_row, 3 * SPAN, 0).reshape(3 * SPAN, KV_HEADS, HEAD)
        value_tile = lax.dynamic_slice_in_dim(value_pad, first_row, 3 * SPAN, 0).reshape(3 * SPAN, KV_HEADS, HEAD)
        places = first_row - SPAN + across
        allowed = inside & (places >= 0) & (places < TOKENS)
        scores = jnp.einsum('qkgd,skd->kgqs', query_tile.astype(jnp.float32), key_tile.astype(jnp.float32)) * HEAD ** (-0.5)
        scores = jnp.where(allowed, scores, -jnp.inf)
        ceiling = jnp.maximum(lax.optimization_barrier(jnp.max(scores, axis=-1, keepdims=True)), sink_rows)
        weights = jnp.exp(scores - ceiling)
        denominator = lax.optimization_barrier(jnp.sum(weights, axis=-1, keepdims=True)) + jnp.exp(sink_rows - ceiling)
        probabilities = (weights / denominator).astype(jnp.bfloat16)
        attended = jnp.einsum('kgqs,skd->qkgd', probabilities.astype(jnp.float32), value_tile.astype(jnp.float32))
        return attended.reshape(SPAN, ATTN_W).astype(jnp.bfloat16)
    return lax.map(one_block, jnp.arange(block_count, dtype=jnp.int32)).reshape(TOKENS, ATTN_W)

def convolve(padded, taps_all, row_count):
    summed = jnp.zeros((row_count, padded.shape[1]), jnp.float32)
    for tap_index in range(CONV):
        summed = summed + padded[tap_index:tap_index + row_count].astype(jnp.float32) * taps_all[tap_index].astype(jnp.float32)
    return jax.nn.silu(summed).astype(jnp.bfloat16)

def sweep(scan_rows, step_rows, decay_rows, write_rows, read_rows):
    per_group = SSD_HEADS // GROUPS
    block_count = TOKENS // SPAN
    highest = lax.Precision.HIGHEST
    scan_tiles = scan_rows.reshape(block_count, SPAN, GROUPS, per_group, SSD_HEAD)
    step_tiles = step_rows.reshape(block_count, SPAN, GROUPS, per_group)
    decay_tiles = decay_rows.reshape(block_count, SPAN, GROUPS, per_group)
    write_tiles = write_rows.reshape(block_count, SPAN, GROUPS, STATE)
    read_tiles = read_rows.reshape(block_count, SPAN, GROUPS, STATE)
    earlier_mask = jnp.arange(SPAN)[:, None] >= jnp.arange(SPAN)[None, :]

    def advance(carried, block_item):
        scan_tile, step_tile, decay_tile, write_tile, read_tile = block_item
        scaled = scan_tile.astype(jnp.float32) * step_tile[..., None]
        write_values = write_tile.astype(jnp.float32)
        read_values = read_tile.astype(jnp.float32)
        running = jnp.cumsum(decay_tile, axis=0)
        spread = running[:, None] - running[None, :]
        fading = jnp.exp(jnp.where(earlier_mask[:, :, None, None], spread, -jnp.inf))
        affinity = jnp.einsum('lgn,sgn->lsg', read_values, write_values, precision=highest)
        within_block = jnp.einsum('lsgr,sgrp->lgrp', affinity[..., None] * fading, scaled, precision=highest)
        from_before = jnp.einsum('lgn,grpn->lgrp', read_values, carried, precision=highest) * jnp.exp(running)[..., None]
        to_end = jnp.exp(running[-1:] - running)
        block_states = jnp.einsum('lgn,lgrp->grpn', write_values, scaled * to_end[..., None], precision=highest)
        return (carried * jnp.exp(running[-1])[..., None, None] + block_states, within_block + from_before)
    start_state = jnp.zeros((GROUPS, per_group, SSD_HEAD, STATE), jnp.float32)
    final_state, outputs = lax.scan(advance, start_state, (scan_tiles, step_tiles, decay_tiles, write_tiles, read_tiles))
    return outputs.reshape(TOKENS, SSD_W)

def reference(asking_matrix, matching_key_matrix, carried_value_matrix, silu_switch_argument, duality_source_matrix, storing_direction_matrix, fetching_direction_matrix, duality_kernel_coefficients, storing_kernel_coefficients, fetching_kernel_coefficients, raw_increment_lengths, logarithmic_fading_speeds, token_fading_spikes, absorber_score_vector, cluster_scaling_factor, final_mapping_matrix):
    attended = attend(rotate(asking_matrix, 0), rotate(matching_key_matrix, 0), carried_value_matrix, absorber_score_vector)
    margin = CONV // 2
    raw_rows = jnp.concatenate([duality_source_matrix, storing_direction_matrix, fetching_direction_matrix], axis=1)
    padded = jnp.pad(raw_rows, ((margin, margin), (0, 0)))
    conved = convolve(padded, jnp.concatenate([duality_kernel_coefficients, storing_kernel_coefficients, fetching_kernel_coefficients], axis=1), TOKENS)
    per_group = SSD_HEADS // GROUPS
    scan_rows = conved[:, :SSD_W].reshape(TOKENS, GROUPS, per_group, SSD_HEAD)
    write_rows = conved[:, SSD_W:SSD_W + GROUPS * STATE].reshape(TOKENS, GROUPS, STATE)
    read_rows = conved[:, SSD_W + GROUPS * STATE:].reshape(TOKENS, GROUPS, STATE)
    joint_increment_lengths = jax.nn.softplus(raw_increment_lengths)
    joint_fading_amounts = -jnp.exp(logarithmic_fading_speeds)[:, :, None] * joint_increment_lengths + token_fading_spikes
    steps_rows = jnp.transpose(joint_increment_lengths, (0, 2, 1)).reshape(2, TOKENS, GROUPS, per_group)
    decay_rows = jnp.transpose(joint_fading_amounts, (0, 2, 1)).reshape(2, TOKENS, GROUPS, per_group)
    ahead_rows = sweep(scan_rows, steps_rows[0], decay_rows[0], write_rows, read_rows)
    back_rows = sweep(scan_rows[::-1], steps_rows[1][::-1], decay_rows[1][::-1], write_rows[::-1], read_rows[::-1])[::-1]
    gated_rows = (ahead_rows + back_rows) * jax.nn.silu(silu_switch_argument.astype(jnp.float32))
    grouped = gated_rows.reshape(TOKENS, GROUPS, SSD_W // GROUPS)
    grouped = grouped * lax.rsqrt(lax.optimization_barrier(jnp.mean(grouped * grouped, axis=-1, keepdims=True)) + EPSILON)
    normed = (grouped.reshape(TOKENS, SSD_W) * cluster_scaling_factor).astype(jnp.bfloat16)
    slice_width = ATTN_W // N_TP
    summed = jnp.zeros((TOKENS, D), jnp.float32)
    for shard_index in range(N_TP):
        first_col = shard_index * slice_width
        partial_sum = jnp.dot(attended[:, first_col:first_col + slice_width], final_mapping_matrix[0, first_col:first_col + slice_width], preferred_element_type=jnp.float32)
        partial_sum = partial_sum + jnp.dot(normed[:, first_col:first_col + slice_width], final_mapping_matrix[1, first_col:first_col + slice_width], preferred_element_type=jnp.float32)
        rounded = lax.optimization_barrier(partial_sum.astype(jnp.bfloat16))
        summed = summed + rounded.astype(jnp.float32)
    return summed.astype(jnp.bfloat16)
```

```python
import functools

import jax
import jax.numpy as jnp
from jax import lax
from jax.experimental import pallas as pl
from jax.experimental.pallas import tpu as pltpu
from jax.sharding import PartitionSpec as P

HEAD = 128
SSD_HEAD = 64
STATE = 128
CONV = 5
WINDOW = 128
SPAN = 128


ROTARY_BASE = 500000.0
EPSILON = 1e-06


def padded_2(cells, sides, width):
    for axis, dim in sides:
        count = lax.axis_size(axis)
        ends = count - 1
        head = lax.slice_in_dim(cells, 0, width, axis=dim)
        tail = lax.slice_in_dim(cells, cells.shape[dim] - width, cells.shape[dim], axis=dim)
        cells = jnp.concatenate(
            [
                lax.ppermute(tail, axis, [(i, (i + 1) % count) for i in range(ends)]),
                cells,
                lax.ppermute(head, axis, [((i + 1) % count, i) for i in range(ends)]),
            ],
            axis=dim,
        )
    return cells


def clique_of(count):
    return 4 if count % 4 == 0 else (2 if count % 2 == 0 else 1)


def greet(partners):
    barrier = pltpu.get_barrier_semaphore()
    for partner in partners:
        pl.semaphore_signal(
            barrier, inc=1, device_id=partner, device_id_type=pl.DeviceIdType.MESH
        )
    pl.semaphore_wait(barrier, len(partners))


def sending(source, target, send_sem, recv_sem, partner):
    return pltpu.make_async_remote_copy(
        src_ref=source,
        dst_ref=target,
        send_sem=send_sem,
        recv_sem=recv_sem,
        device_id=partner,
        device_id_type=pl.DeviceIdType.MESH,
    )


def scan_kernel(
    clique,
    outer,
    state_ref,
    decay_ref,
    out_ref,
    near,
    near_decay,
    prefix,
    before,
    whole,
    whole_decay,
    far,
    far_decay,
    carry,
    replies,
    near_sems,
    far_sems,
    reply_sems,
):
    me = lax.axis_index("sp")
    spot = lax.rem(me, clique)
    layer = me // clique
    base = me - spot
    mates = [lax.rem(spot + d, clique) for d in range(1, clique)]
    layers = [lax.rem(layer + d, outer) for d in range(1, outer)]
    greet(
        [{"sp": base + mate} for mate in mates]
        + [{"sp": other * clique + spot} for other in layers]
    )

    def near_copy(mate, slot, sem_slot):
        who = {"sp": base + mate}
        return (
            sending(
                state_ref.at[mate],
                near.at[slot],
                near_sems.at[0, mate],
                near_sems.at[1, sem_slot],
                who,
            ),
            sending(
                decay_ref.at[mate],
                near_decay.at[slot],
                near_sems.at[2, mate],
                near_sems.at[3, sem_slot],
                who,
            ),
        )

    for mate in mates:
        for copy in near_copy(mate, spot, spot):
            copy.start()
    near[spot] = state_ref[spot]
    near_decay[spot] = decay_ref[spot]
    for mate in mates:
        for copy in near_copy(mate, mate, mate):
            copy.wait_recv()
    for way in range(2):
        order = range(clique) if way == 0 else range(clique - 1, -1, -1)
        running = jnp.zeros(prefix.shape[2:], jnp.float32)
        product = jnp.ones(before.shape[2:], jnp.float32)
        for turn in order:
            prefix[turn, way] = running
            before[turn, way] = product
            factor = near_decay[turn, way]
            running = running * factor[:, None, :] + near[turn, way].astype(jnp.float32)
            product = product * factor
        whole[way] = running.astype(jnp.bfloat16)
        whole_decay[way] = product

    def far_copy(way, other, slot):
        who = {"sp": other * clique + spot}
        return (
            sending(
                whole.at[way],
                far.at[way, slot],
                far_sems.at[0, way, other],
                far_sems.at[1, way, slot],
                who,
            ),
            sending(
                whole_decay.at[way],
                far_decay.at[way, slot],
                far_sems.at[2, way, other],
                far_sems.at[3, way, slot],
                who,
            ),
        )

    def later(way, first, second):
        return second > first if way == 0 else second < first

    for other in layers:
        for way in range(2):

            @pl.when(later(way, layer, other))
            def _():
                for copy in far_copy(way, other, layer):
                    copy.start()

    carry[...] = jnp.zeros_like(carry)
    for way in range(2):
        order = range(outer) if way == 0 else range(outer - 1, -1, -1)
        for other in order:

            @pl.when(later(way, other, layer))
            def _():
                for copy in far_copy(way, other, other):
                    copy.wait_recv()
                carry[way] = carry[way] * far_decay[way, other][:, None, :] + far[
                    way, other
                ].astype(jnp.float32)

    for turn in range(clique):
        for way in range(2):
            replies[turn, way] = (
                prefix[turn, way] + carry[way] * before[turn, way][:, None, :]
            ).astype(jnp.bfloat16)

    def reply(mate, slot):
        return sending(
            replies.at[mate],
            out_ref.at[slot],
            reply_sems.at[0, mate],
            reply_sems.at[1, slot],
            {"sp": base + mate},
        )

    for mate in mates:
        reply(mate, spot).start()
    out_ref[spot] = replies[spot]
    for mate in mates:
        reply(mate, mate).wait_recv()
    for mate in mates:
        for copy in near_copy(mate, spot, spot):
            copy.wait_send()
        reply(mate, spot).wait_send()
    for other in layers:
        for way in range(2):

            @pl.when(later(way, layer, other))
            def _():
                for copy in far_copy(way, other, layer):
                    copy.wait_send()


def scan_states(states, decays):
    count = lax.axis_size("sp")
    clique = clique_of(count)
    outer = count // clique
    ways, heads, rows, cols = states.shape
    part = heads // clique
    states = states.reshape(ways, clique, part, rows, cols).transpose(1, 0, 2, 3, 4)
    decays = jnp.broadcast_to(
        decays.reshape(ways, clique, part).transpose(1, 0, 2)[..., None],
        (clique, ways, part, cols),
    )
    block = (part, rows, cols)
    whole_out = pl.pallas_call(
        functools.partial(scan_kernel, clique, outer),
        out_shape=jax.ShapeDtypeStruct((clique, ways) + block, jnp.bfloat16),
        in_specs=[pl.BlockSpec(memory_space=pltpu.VMEM)] * 2,
        out_specs=pl.BlockSpec(memory_space=pltpu.VMEM),
        scratch_shapes=[
            pltpu.VMEM((clique, ways) + block, jnp.bfloat16),
            pltpu.VMEM((clique, ways, part, cols), jnp.float32),
            pltpu.VMEM((clique, ways) + block, jnp.float32),
            pltpu.VMEM((clique, ways, part, cols), jnp.float32),
            pltpu.VMEM((ways,) + block, jnp.bfloat16),
            pltpu.VMEM((ways, part, cols), jnp.float32),
            pltpu.VMEM((ways, outer) + block, jnp.bfloat16),
            pltpu.VMEM((ways, outer, part, cols), jnp.float32),
            pltpu.VMEM((ways,) + block, jnp.float32),
            pltpu.VMEM((clique, ways) + block, jnp.bfloat16),
            pltpu.SemaphoreType.DMA((4, clique)),
            pltpu.SemaphoreType.DMA((4, 2, outer)),
            pltpu.SemaphoreType.DMA((2, clique)),
        ],
        compiler_params=pltpu.CompilerParams(collective_id=1, has_side_effects=True),
    )(states.astype(jnp.bfloat16), decays)
    return whole_out.transpose(1, 0, 2, 3, 4).reshape(ways, heads, rows, cols)


def project_kernel(
    clique,
    outer,
    tps,
    mixed_ref,
    *rest,
):
    weight_refs = rest[:clique]
    (
        out_ref,
        gathered,
        partial,
        pieces,
        summed,
        mixed_sems,
        piece_sems,
        out_sems,
    ) = rest[clique:]
    me = lax.axis_index("sp")
    lane = lax.axis_index("tp")
    spot = lax.rem(me, clique)
    layer = me // clique
    layers = [lax.rem(layer + d, outer) for d in range(1, outer)]
    lanes = [lax.rem(lane + d, tps) for d in range(1, tps)]

    def at_layer(other):
        return {"sp": other * clique + spot}

    greet([at_layer(other) for other in layers] + [{"tp": other} for other in lanes])
    share = mixed_ref.shape[1] // tps

    def mixed_copy(other, slot):
        return sending(
            mixed_ref,
            gathered.at[slot],
            mixed_sems.at[0, other],
            mixed_sems.at[1, slot],
            at_layer(other),
        )

    def piece_copy(block, other, slot):
        return sending(
            partial.at[block, other],
            pieces.at[block, slot],
            piece_sems.at[0, block, other],
            piece_sems.at[1, block, slot],
            {"tp": other},
        )

    def out_copy(other, slot):
        return sending(
            summed.at[other],
            out_ref.at[slot],
            out_sems.at[0, other],
            out_sems.at[1, slot],
            at_layer(other),
        )

    for other in layers:
        mixed_copy(other, layer).start()
    gathered[layer] = mixed_ref[...]
    order = [layer] + [lax.rem(layer + outer - d, outer) for d in range(1, outer)]

    def multiply(block):
        for flip, weight_ref in enumerate(weight_refs):
            column = flipped(spot, flip)
            product = jnp.dot(
                gathered[block, 0], weight_ref[0], preferred_element_type=jnp.float32
            ) + jnp.dot(
                gathered[block, 1], weight_ref[1], preferred_element_type=jnp.float32
            )
            rounded = product.astype(jnp.bfloat16)
            for other in range(tps):
                partial[block, other, column] = rounded[other * share : (other + 1) * share]
        for other in lanes:
            piece_copy(block, other, lane).start()

    def settle(block, own):
        total = partial[block, lane].astype(jnp.float32)
        for other in lanes:
            piece_copy(block, other, other).wait_recv()
            total = total + pieces[block, other].astype(jnp.float32)
        summed[block] = total.astype(jnp.bfloat16)
        if own:
            out_ref[layer] = summed[layer]
        else:
            out_copy(block, layer).start()

    for turn, block in enumerate(order):
        if turn:
            mixed_copy(block, block).wait_recv()
        multiply(block)
        if turn:
            settle(order[turn - 1], turn == 1)
    settle(order[-1], outer == 1)
    for other in layers:
        out_copy(other, other).wait_recv()
    for other in layers:
        mixed_copy(other, layer).wait_send()
        out_copy(other, layer).wait_send()
    for block in order:
        for other in lanes:
            piece_copy(block, other, lane).wait_send()


def clique_weights(weight):
    count = lax.axis_size("sp")
    clique = clique_of(count)
    held = [weight]
    steps = []
    step = clique // 2
    while step:
        pairs = [(i, (i // clique) * clique + ((i % clique) ^ step)) for i in range(count)]
        held = held + [lax.ppermute(block, "sp", pairs) for block in held]
        steps = steps + [step] if steps else [step]
        step //= 2
    flips = [0]
    for step in steps:
        flips = flips + [flip ^ step for flip in flips]
    return [block for _, block in sorted(zip(flips, held), key=lambda item: item[0])]


def flipped(spot, flip):
    bit = 1
    while bit <= flip:
        if flip & bit:
            spot = spot + bit - 2 * bit * lax.rem(spot // bit, 2)
        bit *= 2
    return spot


def project(mixed, weights):
    count = lax.axis_size("sp")
    tps = lax.axis_size("tp")
    clique = clique_of(count)
    outer = count // clique
    rows = mixed.shape[1]
    width = weights[0].shape[2]
    share = rows // tps
    out = pl.pallas_call(
        functools.partial(project_kernel, clique, outer, tps),
        out_shape=jax.ShapeDtypeStruct((outer, clique, share, width), jnp.bfloat16),
        in_specs=[pl.BlockSpec(memory_space=pltpu.VMEM)] * (1 + clique),
        out_specs=pl.BlockSpec(memory_space=pltpu.VMEM),
        scratch_shapes=[
            pltpu.VMEM((outer,) + mixed.shape, jnp.bfloat16),
            pltpu.VMEM((outer, tps, clique, share, width), jnp.bfloat16),
            pltpu.VMEM((outer, tps, clique, share, width), jnp.bfloat16),
            pltpu.VMEM((outer, clique, share, width), jnp.bfloat16),
            pltpu.SemaphoreType.DMA((2, outer)),
            pltpu.SemaphoreType.DMA((2, outer, tps)),
            pltpu.SemaphoreType.DMA((2, outer)),
        ],
        compiler_params=pltpu.CompilerParams(collective_id=2, has_side_effects=True),
    )(mixed, *weights)
    return out.transpose(2, 0, 1, 3).reshape(share, outer * clique * width)


def rotate(matrix, offset):
    row_count = matrix.shape[0]
    halfway = HEAD // 2
    heads_here = matrix.shape[1] // HEAD
    spacing = ROTARY_BASE ** (-jnp.arange(halfway, dtype=jnp.float32) * 2.0 / HEAD)
    places = (offset + jnp.arange(row_count, dtype=jnp.int32)).astype(jnp.float32)
    angles = places[:, None] * spacing[None, :]
    cosine = jnp.cos(angles)[:, None, :]
    sine_table = jnp.sin(angles)[:, None, :]
    halves = matrix.astype(jnp.float32).reshape(row_count, heads_here, 2, halfway)
    former = halves[:, :, 0]
    latter = halves[:, :, 1]
    turned = jnp.stack(
        [former * cosine - latter * sine_table, latter * cosine + former * sine_table], axis=2
    )
    return turned.reshape(row_count, heads_here * HEAD).astype(jnp.bfloat16)


def banded(matrix, block_count, kv_here):
    stacked = matrix.reshape(block_count + 2, SPAN, kv_here, HEAD)
    return jnp.concatenate([stacked[:-2], stacked[1:-1], stacked[2:]], axis=1)


def attend(turned_queries, key_band, value_band, absorber_score_vector, offset, seq_total):
    row_count = turned_queries.shape[0]
    block_count = row_count // SPAN
    kv_here = key_band.shape[1] // HEAD
    sharing = turned_queries.shape[1] // HEAD // kv_here
    key_tiles = banded(key_band, block_count, kv_here)
    value_tiles = banded(value_band, block_count, kv_here)
    query_tiles = turned_queries.reshape(block_count, SPAN, kv_here, sharing, HEAD)
    scores = jnp.einsum(
        "bqkgd,bskd->bkgqs", query_tiles, key_tiles, preferred_element_type=jnp.float32
    ) * HEAD ** (-0.5)
    within = jnp.arange(SPAN, dtype=jnp.int32)[:, None]
    across = jnp.arange(3 * SPAN, dtype=jnp.int32)[None, :]
    inside = jnp.abs(across - SPAN - within) <= WINDOW
    places = offset - SPAN + jnp.arange(block_count, dtype=jnp.int32)[:, None] * SPAN + across
    present = (places >= 0) & (places < seq_total)
    allowed = inside[None, :, :] & present[:, None, :]
    scores = jnp.where(allowed[:, None, None, :, :], scores, -jnp.inf)
    sink_rows = absorber_score_vector.reshape(kv_here, sharing)[None, :, :, None, None]
    ceiling = jnp.maximum(jnp.max(scores, axis=-1, keepdims=True), sink_rows)
    weights = jnp.exp(scores - ceiling)
    denominator = jnp.sum(weights, axis=-1, keepdims=True) + jnp.exp(sink_rows - ceiling)
    probabilities = (weights / denominator).astype(jnp.bfloat16)
    attended = jnp.einsum(
        "bkgqs,bskd->bqkgd", probabilities, value_tiles, preferred_element_type=jnp.float32
    )
    return attended.reshape(row_count, turned_queries.shape[1]).astype(jnp.bfloat16)


def convolve(padded, taps_all, row_count):
    summed = jnp.zeros((row_count, padded.shape[1]), jnp.float32)
    for tap_index in range(CONV):
        summed = summed + padded[tap_index : tap_index + row_count].astype(jnp.float32) * taps_all[
            tap_index
        ].astype(jnp.float32)
    return jax.nn.silu(summed).astype(jnp.bfloat16)


def prepare(scan_rows, step_rows, decay_rows, write_rows, read_rows):
    row_count = scan_rows.shape[0]
    block_count = row_count // SPAN
    groups_here = write_rows.shape[1]
    per_group = scan_rows.shape[2]
    step_tiles = step_rows.reshape(block_count, SPAN, groups_here, per_group)
    scaled = (
        scan_rows.astype(jnp.float32).reshape(block_count, SPAN, groups_here, per_group, SSD_HEAD)
        * step_tiles[..., None]
    )
    running = jnp.cumsum(decay_rows.reshape(block_count, SPAN, groups_here, per_group), axis=1)
    write_tiles = write_rows.reshape(block_count, SPAN, groups_here, STATE)
    read_tiles = read_rows.reshape(block_count, SPAN, groups_here, STATE)
    earlier_mask = jnp.arange(SPAN)[:, None] >= jnp.arange(SPAN)[None, :]
    spread = running[:, :, None] - running[:, None, :]
    fading = jnp.exp(jnp.where(earlier_mask[None, :, :, None, None], spread, -jnp.inf))
    affinity = jnp.einsum(
        "blgn,bsgn->blsg", read_tiles, write_tiles, preferred_element_type=jnp.float32
    )
    within_block = jnp.einsum(
        "blsgr,bsgrp->blgrp", affinity[..., None] * fading, scaled
    )
    to_end = jnp.exp(running[:, -1:] - running)
    block_states = jnp.einsum(
        "blgn,blgrp->bgrpn",
        write_tiles.astype(jnp.float32),
        scaled * to_end[..., None],
    )
    totals = running[:, -1]

    def advance(carried, block_item):
        fresh_state, block_total = block_item
        return (carried * jnp.exp(block_total)[..., None, None] + fresh_state, carried)

    final_state, entering = lax.scan(
        advance, jnp.zeros(block_states.shape[1:], jnp.float32), (block_states, totals)
    )
    summary = (jnp.exp(jnp.sum(totals, axis=0)), final_state)
    return ((within_block, entering, running, totals, read_tiles), summary)


def finish(pieces, incoming):
    within_block, entering, running, totals, read_tiles = pieces
    before = jnp.cumsum(totals, axis=0) - totals
    starting = entering + incoming[None] * jnp.exp(before)[..., None, None]
    carried = (
        jnp.einsum(
            "blgn,bgrpn->blgrp",
            read_tiles.astype(jnp.float32),
            starting,
        )
        * jnp.exp(running)[..., None]
    )
    joined = within_block + carried
    return joined.reshape(joined.shape[0] * SPAN, -1)


def local(
    asking_matrix,
    matching_key_matrix,
    carried_value_matrix,
    silu_switch_argument,
    duality_source_matrix,
    storing_direction_matrix,
    fetching_direction_matrix,
    duality_kernel_coefficients,
    storing_kernel_coefficients,
    fetching_kernel_coefficients,
    raw_increment_lengths,
    logarithmic_fading_speeds,
    token_fading_spikes,
    absorber_score_vector,
    cluster_scaling_factor,
    final_mapping_matrix,
):
    row_count = asking_matrix.shape[0]
    offset = lax.axis_index("sp") * row_count
    seq_total = lax.axis_size("sp") * row_count
    weights = clique_weights(final_mapping_matrix)
    turned_queries = rotate(asking_matrix, offset)
    key_value = jnp.concatenate([rotate(matching_key_matrix, offset), carried_value_matrix], axis=1)
    raw_rows = jnp.concatenate(
        [duality_source_matrix, storing_direction_matrix, fetching_direction_matrix], axis=1
    )
    margin = CONV // 2
    pair_rims = padded_2(key_value, (("sp", 0),), WINDOW)
    raw_rims = padded_2(raw_rows, (("sp", 0),), margin)
    filler = jnp.zeros((SPAN - WINDOW, key_value.shape[1]), jnp.bfloat16)
    pair_band = jnp.concatenate([filler, pair_rims, filler], axis=0)
    kv_width = matching_key_matrix.shape[1]
    attended = attend(
        turned_queries,
        pair_band[:, :kv_width],
        pair_band[:, kv_width:],
        absorber_score_vector,
        offset,
        seq_total,
    )
    conved = convolve(
        raw_rims,
        jnp.concatenate(
            [
                duality_kernel_coefficients,
                storing_kernel_coefficients,
                fetching_kernel_coefficients,
            ],
            axis=1,
        ),
        row_count,
    )
    scan_width = duality_source_matrix.shape[1]
    write_width = storing_direction_matrix.shape[1]
    groups_here = write_width // STATE
    per_group = scan_width // SSD_HEAD // groups_here
    scan_rows = conved[:, :scan_width].reshape(row_count, groups_here, per_group, SSD_HEAD)
    write_rows = conved[:, scan_width : scan_width + write_width].reshape(
        row_count, groups_here, STATE
    )
    read_rows = conved[:, scan_width + write_width :].reshape(row_count, groups_here, STATE)
    joint_increment_lengths = jax.nn.softplus(raw_increment_lengths)
    joint_fading_amounts = (
        -jnp.exp(logarithmic_fading_speeds)[:, :, None] * joint_increment_lengths
        + token_fading_spikes
    )
    steps_rows = jnp.transpose(joint_increment_lengths, (0, 2, 1)).reshape(
        2, row_count, groups_here, per_group
    )
    decay_rows = jnp.transpose(joint_fading_amounts, (0, 2, 1)).reshape(
        2, row_count, groups_here, per_group
    )
    ahead_pieces, ahead_summary = prepare(
        scan_rows, steps_rows[0], decay_rows[0], write_rows, read_rows
    )
    back_pieces, back_summary = prepare(
        scan_rows[::-1], steps_rows[1][::-1], decay_rows[1][::-1], write_rows[::-1], read_rows[::-1]
    )
    heads = groups_here * per_group
    incoming = scan_states(
        jnp.stack([ahead_summary[1], back_summary[1]]).reshape(2, heads, SSD_HEAD, STATE),
        jnp.stack([ahead_summary[0], back_summary[0]]).reshape(2, heads),
    ).reshape(2, groups_here, per_group, SSD_HEAD, STATE)
    both_ways = finish(ahead_pieces, incoming[0].astype(jnp.float32)) + finish(
        back_pieces, incoming[1].astype(jnp.float32)
    )[::-1]
    gated_rows = both_ways * jax.nn.silu(silu_switch_argument.astype(jnp.float32))
    grouped = gated_rows.reshape(row_count, groups_here, -1)
    grouped = grouped * lax.rsqrt(jnp.mean(grouped * grouped, axis=-1, keepdims=True) + EPSILON)
    normed = (grouped.reshape(row_count, scan_width) * cluster_scaling_factor).astype(jnp.bfloat16)
    return project(jnp.stack([attended, normed]), weights)


def solution(mesh):
    in_specs = (
        P("sp", "tp"),
        P("sp", "tp"),
        P("sp", "tp"),
        P("sp", "tp"),
        P("sp", "tp"),
        P("sp", "tp"),
        P("sp", "tp"),
        P(None, "tp"),
        P(None, "tp"),
        P(None, "tp"),
        P(None, "tp", "sp"),
        P(None, "tp"),
        P(None, "tp", "sp"),
        P("tp"),
        P("tp"),
        P(None, "tp", "sp"),
    )
    out_specs = P(("sp", "tp"), None)
    return jax.shard_map(local, mesh=mesh, in_specs=in_specs, out_specs=out_specs, check_vma=False)
```

```python
import functools

import jax
import jax.numpy as jnp
from jax import lax
from jax.experimental import pallas as pl
from jax.experimental.pallas import tpu as pltpu
from jax.sharding import PartitionSpec as P

HEAD = 128
SSD_HEAD = 64
STATE = 128
CONV = 5
WINDOW = 128
SPAN = 128


ROTARY_BASE = 500000.0
EPSILON = 1e-06


def padded_2(cells, sides, width):
    for axis, dim in sides:
        count = lax.axis_size(axis)
        ends = count - 1
        head = lax.slice_in_dim(cells, 0, width, axis=dim)
        tail = lax.slice_in_dim(cells, cells.shape[dim] - width, cells.shape[dim], axis=dim)
        cells = jnp.concatenate(
            [
                lax.ppermute(tail, axis, [(i, (i + 1) % count) for i in range(ends)]),
                cells,
                lax.ppermute(head, axis, [((i + 1) % count, i) for i in range(ends)]),
            ],
            axis=dim,
        )
    return cells


def clique_of(count):
    return 4 if count % 4 == 0 else (2 if count % 2 == 0 else 1)


def greet(partners):
    barrier = pltpu.get_barrier_semaphore()
    for partner in partners:
        pl.semaphore_signal(
            barrier, inc=1, device_id=partner, device_id_type=pl.DeviceIdType.MESH
        )
    pl.semaphore_wait(barrier, len(partners))


def sending(source, target, send_sem, recv_sem, partner):
    return pltpu.make_async_remote_copy(
        src_ref=source,
        dst_ref=target,
        send_sem=send_sem,
        recv_sem=recv_sem,
        device_id=partner,
        device_id_type=pl.DeviceIdType.MESH,
    )


def scan_kernel(
    clique,
    outer,
    state_ref,
    decay_ref,
    weight_ref,
    out_ref,
    onward_ref,
    near,
    near_decay,
    prefix,
    before,
    whole,
    whole_decay,
    far,
    far_decay,
    carry,
    replies,
    near_sems,
    far_sems,
    reply_sems,
    ring_sems,
):
    me = lax.axis_index("sp")
    spot = lax.rem(me, clique)
    layer = me // clique
    base = me - spot
    mates = [lax.rem(spot + d, clique) for d in range(1, clique)]
    layers = [lax.rem(layer + d, outer) for d in range(1, outer)]
    greet(
        [{"sp": base + mate} for mate in mates]
        + [{"sp": other * clique + spot} for other in layers]
    )

    ring = sending(
        weight_ref,
        onward_ref,
        ring_sems.at[0],
        ring_sems.at[1],
        {"sp": lax.rem(layer + 1, outer) * clique + spot},
    )
    if outer > 1:
        ring.start()

    def near_copy(mate, slot, sem_slot):
        who = {"sp": base + mate}
        return (
            sending(
                state_ref.at[mate],
                near.at[slot],
                near_sems.at[0, mate],
                near_sems.at[1, sem_slot],
                who,
            ),
            sending(
                decay_ref.at[mate],
                near_decay.at[slot],
                near_sems.at[2, mate],
                near_sems.at[3, sem_slot],
                who,
            ),
        )

    for mate in mates:
        for copy in near_copy(mate, spot, spot):
            copy.start()
    near[spot] = state_ref[spot]
    near_decay[spot] = decay_ref[spot]
    for mate in mates:
        for copy in near_copy(mate, mate, mate):
            copy.wait_recv()
    for way in range(2):
        order = range(clique) if way == 0 else range(clique - 1, -1, -1)
        running = jnp.zeros(prefix.shape[2:], jnp.float32)
        product = jnp.ones(before.shape[2:], jnp.float32)
        for turn in order:
            prefix[turn, way] = running
            before[turn, way] = product
            factor = near_decay[turn, way]
            running = running * factor[:, None, :] + near[turn, way].astype(jnp.float32)
            product = product * factor
        whole[way] = running.astype(jnp.bfloat16)
        whole_decay[way] = product

    def far_copy(way, other, slot):
        who = {"sp": other * clique + spot}
        return (
            sending(
                whole.at[way],
                far.at[way, slot],
                far_sems.at[0, way, other],
                far_sems.at[1, way, slot],
                who,
            ),
            sending(
                whole_decay.at[way],
                far_decay.at[way, slot],
                far_sems.at[2, way, other],
                far_sems.at[3, way, slot],
                who,
            ),
        )

    def later(way, first, second):
        return second > first if way == 0 else second < first

    for other in layers:
        for way in range(2):

            @pl.when(later(way, layer, other))
            def _():
                for copy in far_copy(way, other, layer):
                    copy.start()

    carry[...] = jnp.zeros_like(carry)
    for way in range(2):
        order = range(outer) if way == 0 else range(outer - 1, -1, -1)
        for other in order:

            @pl.when(later(way, other, layer))
            def _():
                for copy in far_copy(way, other, other):
                    copy.wait_recv()
                carry[way] = carry[way] * far_decay[way, other][:, None, :] + far[
                    way, other
                ].astype(jnp.float32)

    for turn in range(clique):
        for way in range(2):
            replies[turn, way] = (
                prefix[turn, way] + carry[way] * before[turn, way][:, None, :]
            ).astype(jnp.bfloat16)

    def reply(mate, slot):
        return sending(
            replies.at[mate],
            out_ref.at[slot],
            reply_sems.at[0, mate],
            reply_sems.at[1, slot],
            {"sp": base + mate},
        )

    for mate in mates:
        reply(mate, spot).start()
    out_ref[spot] = replies[spot]
    for mate in mates:
        reply(mate, mate).wait_recv()
    for mate in mates:
        for copy in near_copy(mate, spot, spot):
            copy.wait_send()
        reply(mate, spot).wait_send()
    for other in layers:
        for way in range(2):

            @pl.when(later(way, layer, other))
            def _():
                for copy in far_copy(way, other, layer):
                    copy.wait_send()

    if outer > 1:
        ring.wait()


def scan_states(states, decays, weight):
    count = lax.axis_size("sp")
    clique = clique_of(count)
    outer = count // clique
    ways, heads, rows, cols = states.shape
    part = heads // clique
    states = states.reshape(ways, clique, part, rows, cols).transpose(1, 0, 2, 3, 4)
    decays = jnp.broadcast_to(
        decays.reshape(ways, clique, part).transpose(1, 0, 2)[..., None],
        (clique, ways, part, cols),
    )
    block = (part, rows, cols)
    whole_out, onward = pl.pallas_call(
        functools.partial(scan_kernel, clique, outer),
        out_shape=(
            jax.ShapeDtypeStruct((clique, ways) + block, jnp.bfloat16),
            jax.ShapeDtypeStruct(weight.shape, weight.dtype),
        ),
        in_specs=[pl.BlockSpec(memory_space=pltpu.VMEM)] * 2
        + [pl.BlockSpec(memory_space=pl.ANY)],
        out_specs=(
            pl.BlockSpec(memory_space=pltpu.VMEM),
            pl.BlockSpec(memory_space=pl.ANY),
        ),
        scratch_shapes=[
            pltpu.VMEM((clique, ways) + block, jnp.bfloat16),
            pltpu.VMEM((clique, ways, part, cols), jnp.float32),
            pltpu.VMEM((clique, ways) + block, jnp.float32),
            pltpu.VMEM((clique, ways, part, cols), jnp.float32),
            pltpu.VMEM((ways,) + block, jnp.bfloat16),
            pltpu.VMEM((ways, part, cols), jnp.float32),
            pltpu.VMEM((ways, outer) + block, jnp.bfloat16),
            pltpu.VMEM((ways, outer, part, cols), jnp.float32),
            pltpu.VMEM((ways,) + block, jnp.float32),
            pltpu.VMEM((clique, ways) + block, jnp.bfloat16),
            pltpu.SemaphoreType.DMA((4, clique)),
            pltpu.SemaphoreType.DMA((4, 2, outer)),
            pltpu.SemaphoreType.DMA((2, clique)),
            pltpu.SemaphoreType.DMA((2,)),
        ],
        compiler_params=pltpu.CompilerParams(collective_id=1, has_side_effects=True),
        cost_estimate=pl.CostEstimate(
            flops=0, bytes_accessed=320 * states.size, transcendentals=0
        ),
    )(states.astype(jnp.bfloat16), decays, weight)
    return whole_out.transpose(1, 0, 2, 3, 4).reshape(ways, heads, rows, cols), onward


def project_kernel(clique, outer, tps, mixed_ref, *rest):
    weight_refs = rest[:outer]
    (
        out_ref,
        gathered,
        partial,
        pieces,
        summed,
        mixed_sems,
        piece_sems,
        out_sems,
    ) = rest[outer:]
    me = lax.axis_index("sp")
    lane = lax.axis_index("tp")
    spot = lax.rem(me, clique)
    layer = me // clique
    base = me - spot
    flips = list(range(1, clique))
    lanes = [lax.rem(lane + d, tps) for d in range(1, tps)]

    def at_flip(flip):
        return {"sp": base + flipped(spot, flip)}

    greet([at_flip(flip) for flip in flips] + [{"tp": other} for other in lanes])
    share = mixed_ref.shape[1] // tps

    def mixed_copy(flip):
        low = flip & -flip
        high = flip - low
        return sending(
            gathered.at[high] if high else mixed_ref,
            gathered.at[flip],
            mixed_sems.at[0, flip],
            mixed_sems.at[1, flip],
            at_flip(low),
        )

    def piece_copy(flip, other, slot):
        return sending(
            partial.at[flip, other],
            pieces.at[flip, slot],
            piece_sems.at[0, flip, other],
            piece_sems.at[1, flip, slot],
            {"tp": other},
        )

    def out_copy(flip, slot):
        return sending(
            summed.at[flip],
            out_ref.at[slot],
            out_sems.at[0, flip],
            out_sems.at[1, flip],
            at_flip(flip),
        )

    for flip in reversed(flips):
        if flip & (flip - 1) == 0:
            mixed_copy(flip).start()

    def multiply(flip):
        source = gathered.at[flip] if flip else mixed_ref
        for turn, weight_ref in enumerate(weight_refs):
            column = lax.rem(layer + outer - turn, outer)
            product = jnp.dot(
                source[0], weight_ref[0], preferred_element_type=jnp.float32
            ) + jnp.dot(source[1], weight_ref[1], preferred_element_type=jnp.float32)
            rounded = product.astype(jnp.bfloat16)
            for other in range(tps):
                partial[flip, other, column] = rounded[other * share : (other + 1) * share]
        for other in lanes:
            piece_copy(flip, other, lane).start()

    def settle(flip):
        total = partial[flip, lane].astype(jnp.float32)
        for other in lanes:
            piece_copy(flip, other, other).wait_recv()
            total = total + pieces[flip, other].astype(jnp.float32)
        if flip:
            summed[flip] = total.astype(jnp.bfloat16)
            out_copy(flip, spot).start()
        else:
            out_ref[spot] = total.astype(jnp.bfloat16)

    for flip in range(clique):
        if flip:
            mixed_copy(flip).wait_recv()
            for further in flips:
                if further != flip and further - (further & -further) == flip:
                    mixed_copy(further).start()
        multiply(flip)
        if flip:
            settle(flip - 1)
    settle(clique - 1)
    for flip in flips:
        out_copy(flip, flipped(spot, flip)).wait_recv()
    for flip in flips:
        mixed_copy(flip).wait_send()
        out_copy(flip, spot).wait_send()
    for flip in range(clique):
        for other in lanes:
            piece_copy(flip, other, lane).wait_send()


def ring_weights(held, limit=None):
    count = lax.axis_size("sp")
    clique = clique_of(count)
    outer = count // clique
    pairs = [(i, (i + clique) % count) for i in range(count)]
    held = held[:outer]
    while len(held) < min(limit or outer, outer):
        held = held + [lax.ppermute(held[-1], "sp", pairs)]
    return held


def flipped(spot, flip):
    bit = 1
    while bit <= flip:
        if flip & bit:
            spot = spot + bit - 2 * bit * lax.rem(spot // bit, 2)
        bit *= 2
    return spot


def project(mixed, weights):
    count = lax.axis_size("sp")
    tps = lax.axis_size("tp")
    clique = clique_of(count)
    outer = count // clique
    rows = mixed.shape[1]
    width = weights[0].shape[2]
    share = rows // tps
    block = (outer, share, width)
    out = pl.pallas_call(
        functools.partial(project_kernel, clique, outer, tps),
        out_shape=jax.ShapeDtypeStruct((clique,) + block, jnp.bfloat16),
        in_specs=[pl.BlockSpec(memory_space=pltpu.VMEM)] * (1 + outer),
        out_specs=pl.BlockSpec(memory_space=pltpu.VMEM),
        scratch_shapes=[
            pltpu.VMEM((clique,) + mixed.shape, jnp.bfloat16),
            pltpu.VMEM((clique, tps) + block, jnp.bfloat16),
            pltpu.VMEM((clique, tps) + block, jnp.bfloat16),
            pltpu.VMEM((clique,) + block, jnp.bfloat16),
            pltpu.SemaphoreType.DMA((2, clique)),
            pltpu.SemaphoreType.DMA((2, clique, tps)),
            pltpu.SemaphoreType.DMA((2, clique)),
        ],
        compiler_params=pltpu.CompilerParams(collective_id=2, has_side_effects=True),
    )(mixed, *weights)
    return out.transpose(2, 1, 0, 3).reshape(share, outer * clique * width)


def rotate(matrix, offset):
    row_count = matrix.shape[0]
    halfway = HEAD // 2
    heads_here = matrix.shape[1] // HEAD
    spacing = ROTARY_BASE ** (-jnp.arange(halfway, dtype=jnp.float32) * 2.0 / HEAD)
    places = (offset + jnp.arange(row_count, dtype=jnp.int32)).astype(jnp.float32)
    angles = places[:, None] * spacing[None, :]
    cosine = jnp.cos(angles)[:, None, :]
    sine_table = jnp.sin(angles)[:, None, :]
    halves = matrix.astype(jnp.float32).reshape(row_count, heads_here, 2, halfway)
    former = halves[:, :, 0]
    latter = halves[:, :, 1]
    turned = jnp.stack(
        [former * cosine - latter * sine_table, latter * cosine + former * sine_table], axis=2
    )
    return turned.reshape(row_count, heads_here * HEAD).astype(jnp.bfloat16)


def banded(matrix, block_count, kv_here):
    stacked = matrix.reshape(block_count + 2, SPAN, kv_here, HEAD)
    return jnp.concatenate([stacked[:-2], stacked[1:-1], stacked[2:]], axis=1)


def attend(turned_queries, key_band, value_band, absorber_score_vector, offset, seq_total):
    row_count = turned_queries.shape[0]
    block_count = row_count // SPAN
    kv_here = key_band.shape[1] // HEAD
    sharing = turned_queries.shape[1] // HEAD // kv_here
    key_tiles = banded(key_band, block_count, kv_here)
    value_tiles = banded(value_band, block_count, kv_here)
    query_tiles = turned_queries.reshape(block_count, SPAN, kv_here, sharing, HEAD)
    scores = jnp.einsum(
        "bqkgd,bskd->bkgqs", query_tiles, key_tiles, preferred_element_type=jnp.float32
    ) * HEAD ** (-0.5)
    within = jnp.arange(SPAN, dtype=jnp.int32)[:, None]
    across = jnp.arange(3 * SPAN, dtype=jnp.int32)[None, :]
    inside = jnp.abs(across - SPAN - within) <= WINDOW
    places = offset - SPAN + jnp.arange(block_count, dtype=jnp.int32)[:, None] * SPAN + across
    present = (places >= 0) & (places < seq_total)
    allowed = inside[None, :, :] & present[:, None, :]
    scores = jnp.where(allowed[:, None, None, :, :], scores, -jnp.inf)
    sink_rows = absorber_score_vector.reshape(kv_here, sharing)[None, :, :, None, None]
    ceiling = jnp.maximum(jnp.max(scores, axis=-1, keepdims=True), sink_rows)
    weights = jnp.exp(scores - ceiling)
    denominator = jnp.sum(weights, axis=-1, keepdims=True) + jnp.exp(sink_rows - ceiling)
    probabilities = (weights / denominator).astype(jnp.bfloat16)
    attended = jnp.einsum(
        "bkgqs,bskd->bqkgd", probabilities, value_tiles, preferred_element_type=jnp.float32
    )
    return attended.reshape(row_count, turned_queries.shape[1]).astype(jnp.bfloat16)


def convolve(padded, taps_all, row_count):
    summed = jnp.zeros((row_count, padded.shape[1]), jnp.float32)
    for tap_index in range(CONV):
        summed = summed + padded[tap_index : tap_index + row_count].astype(jnp.float32) * taps_all[
            tap_index
        ].astype(jnp.float32)
    return jax.nn.silu(summed).astype(jnp.bfloat16)


def prepare(scan_rows, step_rows, decay_rows, write_rows, read_rows):
    row_count = scan_rows.shape[0]
    block_count = row_count // SPAN
    groups_here = write_rows.shape[1]
    per_group = scan_rows.shape[2]
    step_tiles = step_rows.reshape(block_count, SPAN, groups_here, per_group)
    scaled = (
        scan_rows.astype(jnp.float32).reshape(block_count, SPAN, groups_here, per_group, SSD_HEAD)
        * step_tiles[..., None]
    )
    running = jnp.cumsum(decay_rows.reshape(block_count, SPAN, groups_here, per_group), axis=1)
    write_tiles = write_rows.reshape(block_count, SPAN, groups_here, STATE)
    read_tiles = read_rows.reshape(block_count, SPAN, groups_here, STATE)
    earlier_mask = jnp.arange(SPAN)[:, None] >= jnp.arange(SPAN)[None, :]
    spread = running[:, :, None] - running[:, None, :]
    fading = jnp.exp(jnp.where(earlier_mask[None, :, :, None, None], spread, -jnp.inf))
    affinity = jnp.einsum(
        "blgn,bsgn->blsg", read_tiles, write_tiles, preferred_element_type=jnp.float32
    )
    within_block = jnp.einsum(
        "blsgr,bsgrp->blgrp", affinity[..., None] * fading, scaled
    )
    to_end = jnp.exp(running[:, -1:] - running)
    block_states = jnp.einsum(
        "blgn,blgrp->bgrpn",
        write_tiles.astype(jnp.float32),
        scaled * to_end[..., None],
    )
    totals = running[:, -1]

    def advance(carried, block_item):
        fresh_state, block_total = block_item
        return (carried * jnp.exp(block_total)[..., None, None] + fresh_state, carried)

    final_state, entering = lax.scan(
        advance, jnp.zeros(block_states.shape[1:], jnp.float32), (block_states, totals)
    )
    summary = (jnp.exp(jnp.sum(totals, axis=0)), final_state)
    return ((within_block, entering, running, totals, read_tiles), summary)


def finish(pieces, incoming):
    within_block, entering, running, totals, read_tiles = pieces
    before = jnp.cumsum(totals, axis=0) - totals
    starting = entering + incoming[None] * jnp.exp(before)[..., None, None]
    carried = (
        jnp.einsum(
            "blgn,bgrpn->blgrp",
            read_tiles.astype(jnp.float32),
            starting,
        )
        * jnp.exp(running)[..., None]
    )
    joined = within_block + carried
    return joined.reshape(joined.shape[0] * SPAN, -1)


def local(
    asking_matrix,
    matching_key_matrix,
    carried_value_matrix,
    silu_switch_argument,
    duality_source_matrix,
    storing_direction_matrix,
    fetching_direction_matrix,
    duality_kernel_coefficients,
    storing_kernel_coefficients,
    fetching_kernel_coefficients,
    raw_increment_lengths,
    logarithmic_fading_speeds,
    token_fading_spikes,
    absorber_score_vector,
    cluster_scaling_factor,
    final_mapping_matrix,
):
    row_count = asking_matrix.shape[0]
    offset = lax.axis_index("sp") * row_count
    seq_total = lax.axis_size("sp") * row_count
    weights = ring_weights([final_mapping_matrix], 2)
    turned_queries = rotate(asking_matrix, offset)
    key_value = jnp.concatenate([rotate(matching_key_matrix, offset), carried_value_matrix], axis=1)
    raw_rows = jnp.concatenate(
        [duality_source_matrix, storing_direction_matrix, fetching_direction_matrix], axis=1
    )
    margin = CONV // 2
    pair_rims = padded_2(key_value, (("sp", 0),), WINDOW)
    raw_rims = padded_2(raw_rows, (("sp", 0),), margin)
    filler = jnp.zeros((SPAN - WINDOW, key_value.shape[1]), jnp.bfloat16)
    pair_band = jnp.concatenate([filler, pair_rims, filler], axis=0)
    kv_width = matching_key_matrix.shape[1]
    conved = convolve(
        raw_rims,
        jnp.concatenate(
            [
                duality_kernel_coefficients,
                storing_kernel_coefficients,
                fetching_kernel_coefficients,
            ],
            axis=1,
        ),
        row_count,
    )
    scan_width = duality_source_matrix.shape[1]
    write_width = storing_direction_matrix.shape[1]
    groups_here = write_width // STATE
    per_group = scan_width // SSD_HEAD // groups_here
    scan_rows = conved[:, :scan_width].reshape(row_count, groups_here, per_group, SSD_HEAD)
    write_rows = conved[:, scan_width : scan_width + write_width].reshape(
        row_count, groups_here, STATE
    )
    read_rows = conved[:, scan_width + write_width :].reshape(row_count, groups_here, STATE)
    joint_increment_lengths = jax.nn.softplus(raw_increment_lengths)
    joint_fading_amounts = (
        -jnp.exp(logarithmic_fading_speeds)[:, :, None] * joint_increment_lengths
        + token_fading_spikes
    )
    steps_rows = jnp.transpose(joint_increment_lengths, (0, 2, 1)).reshape(
        2, row_count, groups_here, per_group
    )
    decay_rows = jnp.transpose(joint_fading_amounts, (0, 2, 1)).reshape(
        2, row_count, groups_here, per_group
    )
    ahead_pieces, ahead_summary = prepare(
        scan_rows, steps_rows[0], decay_rows[0], write_rows, read_rows
    )
    back_pieces, back_summary = prepare(
        scan_rows[::-1], steps_rows[1][::-1], decay_rows[1][::-1], write_rows[::-1], read_rows[::-1]
    )
    heads = groups_here * per_group
    incoming, onward = scan_states(
        jnp.stack([ahead_summary[1], back_summary[1]]).reshape(2, heads, SSD_HEAD, STATE),
        jnp.stack([ahead_summary[0], back_summary[0]]).reshape(2, heads),
        weights[-1],
    )
    weights = ring_weights(weights + [onward])
    incoming = incoming.reshape(2, groups_here, per_group, SSD_HEAD, STATE)
    turned_queries, incoming = lax.optimization_barrier((turned_queries, incoming))
    attended = attend(
        turned_queries,
        pair_band[:, :kv_width],
        pair_band[:, kv_width:],
        absorber_score_vector,
        offset,
        seq_total,
    )
    both_ways = finish(ahead_pieces, incoming[0].astype(jnp.float32)) + finish(
        back_pieces, incoming[1].astype(jnp.float32)
    )[::-1]
    gated_rows = both_ways * jax.nn.silu(silu_switch_argument.astype(jnp.float32))
    grouped = gated_rows.reshape(row_count, groups_here, -1)
    grouped = grouped * lax.rsqrt(jnp.mean(grouped * grouped, axis=-1, keepdims=True) + EPSILON)
    normed = (grouped.reshape(row_count, scan_width) * cluster_scaling_factor).astype(jnp.bfloat16)
    return project(jnp.stack([attended, normed]), weights)


def solution(mesh):
    in_specs = (
        P("sp", "tp"),
        P("sp", "tp"),
        P("sp", "tp"),
        P("sp", "tp"),
        P("sp", "tp"),
        P("sp", "tp"),
        P("sp", "tp"),
        P(None, "tp"),
        P(None, "tp"),
        P(None, "tp"),
        P(None, "tp", "sp"),
        P(None, "tp"),
        P(None, "tp", "sp"),
        P("tp"),
        P("tp"),
        P(None, "tp", "sp"),
    )
    out_specs = P(("sp", "tp"), None)
    return jax.shard_map(local, mesh=mesh, in_specs=in_specs, out_specs=out_specs, check_vma=False)
```

```python
import functools

import jax
import jax.numpy as jnp
from jax import lax
from jax.experimental import pallas as pl
from jax.experimental.pallas import tpu as pltpu
from jax.sharding import PartitionSpec as P

HEAD = 128
SSD_HEAD = 64
STATE = 128
CONV = 5
WINDOW = 128
SPAN = 128


ROTARY_BASE = 500000.0
EPSILON = 1e-06


def padded_2(cells, sides, width):
    for axis, dim in sides:
        count = lax.axis_size(axis)
        ends = count - 1
        head = lax.slice_in_dim(cells, 0, width, axis=dim)
        tail = lax.slice_in_dim(cells, cells.shape[dim] - width, cells.shape[dim], axis=dim)
        cells = jnp.concatenate(
            [
                lax.ppermute(tail, axis, [(i, (i + 1) % count) for i in range(ends)]),
                cells,
                lax.ppermute(head, axis, [((i + 1) % count, i) for i in range(ends)]),
            ],
            axis=dim,
        )
    return cells


def clique_of(count):
    return 4 if count % 4 == 0 else (2 if count % 2 == 0 else 1)


def greet(partners):
    barrier = pltpu.get_barrier_semaphore()
    for partner in partners:
        pl.semaphore_signal(
            barrier, inc=1, device_id=partner, device_id_type=pl.DeviceIdType.MESH
        )
    pl.semaphore_wait(barrier, len(partners))


def sending(source, target, send_sem, recv_sem, partner):
    return pltpu.make_async_remote_copy(
        src_ref=source,
        dst_ref=target,
        send_sem=send_sem,
        recv_sem=recv_sem,
        device_id=partner,
        device_id_type=pl.DeviceIdType.MESH,
    )


def scan_kernel(
    clique,
    outer,
    state_ref,
    decay_ref,
    weight_ref,
    out_ref,
    onward_ref,
    near,
    near_decay,
    prefix,
    before,
    whole,
    whole_decay,
    far,
    far_decay,
    carry,
    replies,
    near_sems,
    far_sems,
    reply_sems,
    ring_sems,
):
    me = lax.axis_index("sp")
    spot = lax.rem(me, clique)
    layer = me // clique
    base = me - spot
    mates = [lax.rem(spot + d, clique) for d in range(1, clique)]
    layers = [lax.rem(layer + d, outer) for d in range(1, outer)]
    greet(
        [{"sp": base + mate} for mate in mates]
        + [{"sp": other * clique + spot} for other in layers]
    )

    ring = sending(
        weight_ref,
        onward_ref,
        ring_sems.at[0],
        ring_sems.at[1],
        {"sp": lax.rem(layer + 1, outer) * clique + spot},
    )
    if outer > 1:
        ring.start()

    def near_copy(mate, slot, sem_slot):
        who = {"sp": base + mate}
        return (
            sending(
                state_ref.at[mate],
                near.at[slot],
                near_sems.at[0, mate],
                near_sems.at[1, sem_slot],
                who,
            ),
            sending(
                decay_ref.at[mate],
                near_decay.at[slot],
                near_sems.at[2, mate],
                near_sems.at[3, sem_slot],
                who,
            ),
        )

    for mate in mates:
        for copy in near_copy(mate, spot, spot):
            copy.start()
    near[spot] = state_ref[spot]
    near_decay[spot] = decay_ref[spot]
    for mate in mates:
        for copy in near_copy(mate, mate, mate):
            copy.wait_recv()
    for way in range(2):
        order = range(clique) if way == 0 else range(clique - 1, -1, -1)
        running = jnp.zeros(prefix.shape[2:], jnp.float32)
        product = jnp.ones(before.shape[2:], jnp.float32)
        for turn in order:
            prefix[turn, way] = running
            before[turn, way] = product
            factor = near_decay[turn, way]
            running = running * factor[:, None, :] + near[turn, way].astype(jnp.float32)
            product = product * factor
        whole[way] = running.astype(jnp.bfloat16)
        whole_decay[way] = product

    def far_copy(way, other, slot):
        who = {"sp": other * clique + spot}
        return (
            sending(
                whole.at[way],
                far.at[way, slot],
                far_sems.at[0, way, other],
                far_sems.at[1, way, slot],
                who,
            ),
            sending(
                whole_decay.at[way],
                far_decay.at[way, slot],
                far_sems.at[2, way, other],
                far_sems.at[3, way, slot],
                who,
            ),
        )

    def later(way, first, second):
        return second > first if way == 0 else second < first

    for other in layers:
        for way in range(2):

            @pl.when(later(way, layer, other))
            def _():
                for copy in far_copy(way, other, layer):
                    copy.start()

    carry[...] = jnp.zeros_like(carry)
    for way in range(2):
        order = range(outer) if way == 0 else range(outer - 1, -1, -1)
        for other in order:

            @pl.when(later(way, other, layer))
            def _():
                for copy in far_copy(way, other, other):
                    copy.wait_recv()
                carry[way] = carry[way] * far_decay[way, other][:, None, :] + far[
                    way, other
                ].astype(jnp.float32)

    for turn in range(clique):
        for way in range(2):
            replies[turn, way] = (
                prefix[turn, way] + carry[way] * before[turn, way][:, None, :]
            ).astype(jnp.bfloat16)

    def reply(mate, slot):
        return sending(
            replies.at[mate],
            out_ref.at[slot],
            reply_sems.at[0, mate],
            reply_sems.at[1, slot],
            {"sp": base + mate},
        )

    for mate in mates:
        reply(mate, spot).start()
    out_ref[spot] = replies[spot]
    for mate in mates:
        reply(mate, mate).wait_recv()
    for mate in mates:
        for copy in near_copy(mate, spot, spot):
            copy.wait_send()
        reply(mate, spot).wait_send()
    for other in layers:
        for way in range(2):

            @pl.when(later(way, layer, other))
            def _():
                for copy in far_copy(way, other, layer):
                    copy.wait_send()

    if outer > 1:
        ring.wait()


def scan_states(states, decays, weight):
    count = lax.axis_size("sp")
    clique = clique_of(count)
    outer = count // clique
    ways, heads, rows, cols = states.shape
    part = heads // clique
    states = states.reshape(ways, clique, part, rows, cols).transpose(1, 0, 2, 3, 4)
    decays = jnp.broadcast_to(
        decays.reshape(ways, clique, part).transpose(1, 0, 2)[..., None],
        (clique, ways, part, cols),
    )
    block = (part, rows, cols)
    whole_out, onward = pl.pallas_call(
        functools.partial(scan_kernel, clique, outer),
        out_shape=(
            jax.ShapeDtypeStruct((clique, ways) + block, jnp.bfloat16),
            jax.ShapeDtypeStruct(weight.shape, weight.dtype),
        ),
        in_specs=[pl.BlockSpec(memory_space=pltpu.VMEM)] * 2
        + [pl.BlockSpec(memory_space=pl.ANY)],
        out_specs=(
            pl.BlockSpec(memory_space=pltpu.VMEM),
            pl.BlockSpec(memory_space=pl.ANY),
        ),
        scratch_shapes=[
            pltpu.VMEM((clique, ways) + block, jnp.bfloat16),
            pltpu.VMEM((clique, ways, part, cols), jnp.float32),
            pltpu.VMEM((clique, ways) + block, jnp.float32),
            pltpu.VMEM((clique, ways, part, cols), jnp.float32),
            pltpu.VMEM((ways,) + block, jnp.bfloat16),
            pltpu.VMEM((ways, part, cols), jnp.float32),
            pltpu.VMEM((ways, outer) + block, jnp.bfloat16),
            pltpu.VMEM((ways, outer, part, cols), jnp.float32),
            pltpu.VMEM((ways,) + block, jnp.float32),
            pltpu.VMEM((clique, ways) + block, jnp.bfloat16),
            pltpu.SemaphoreType.DMA((4, clique)),
            pltpu.SemaphoreType.DMA((4, 2, outer)),
            pltpu.SemaphoreType.DMA((2, clique)),
            pltpu.SemaphoreType.DMA((2,)),
        ],
        compiler_params=pltpu.CompilerParams(collective_id=1, has_side_effects=True),
        cost_estimate=pl.CostEstimate(
            flops=0, bytes_accessed=320 * states.size, transcendentals=0
        ),
    )(states.astype(jnp.bfloat16), decays, weight)
    return whole_out.transpose(1, 0, 2, 3, 4).reshape(ways, heads, rows, cols), onward


def project_kernel(clique, outer, tps, mixed_ref, *rest):
    given = max(outer - 1, 1)
    weight_refs = list(rest[:given])
    (
        out_ref,
        gathered,
        partial,
        pieces,
        summed,
        mixed_sems,
        piece_sems,
        out_sems,
        last,
        ring_sems,
    ) = rest[given:]
    me = lax.axis_index("sp")
    lane = lax.axis_index("tp")
    spot = lax.rem(me, clique)
    layer = me // clique
    base = me - spot
    flips = list(range(1, clique))
    lanes = [lax.rem(lane + d, tps) for d in range(1, tps)]

    def at_flip(flip):
        return {"sp": base + flipped(spot, flip)}

    after = {"sp": lax.rem(layer + 1, outer) * clique + spot}
    prior = {"sp": lax.rem(layer + outer - 1, outer) * clique + spot}
    greet(
        [at_flip(flip) for flip in flips]
        + [{"tp": other} for other in lanes]
        + ([after, prior] if outer > 1 else [])
    )
    ring = sending(weight_refs[-1], last, ring_sems.at[0], ring_sems.at[1], after)
    if outer > 1:
        ring.start()
        weight_refs = weight_refs + [last]
    share = mixed_ref.shape[1] // tps

    def mixed_copy(flip):
        low = flip & -flip
        high = flip - low
        return sending(
            gathered.at[high] if high else mixed_ref,
            gathered.at[flip],
            mixed_sems.at[0, flip],
            mixed_sems.at[1, flip],
            at_flip(low),
        )

    def piece_copy(flip, other, slot):
        return sending(
            partial.at[flip, other],
            pieces.at[flip, slot],
            piece_sems.at[0, flip, other],
            piece_sems.at[1, flip, slot],
            {"tp": other},
        )

    def out_copy(flip, slot):
        return sending(
            summed.at[flip],
            out_ref.at[slot],
            out_sems.at[0, flip],
            out_sems.at[1, flip],
            at_flip(flip),
        )

    for flip in reversed(flips):
        if flip & (flip - 1) == 0:
            mixed_copy(flip).start()

    def multiply(flip, turns):
        source = gathered.at[flip] if flip else mixed_ref
        for turn in turns:
            weight_ref = weight_refs[turn]
            column = lax.rem(layer + outer - turn, outer)
            product = jnp.dot(
                source[0], weight_ref[0], preferred_element_type=jnp.float32
            ) + jnp.dot(source[1], weight_ref[1], preferred_element_type=jnp.float32)
            rounded = product.astype(jnp.bfloat16)
            for other in range(tps):
                partial[flip, other, column] = rounded[other * share : (other + 1) * share]

    def settle(flip):
        total = partial[flip, lane].astype(jnp.float32)
        for other in lanes:
            piece_copy(flip, other, other).wait_recv()
            total = total + pieces[flip, other].astype(jnp.float32)
        if flip:
            summed[flip] = total.astype(jnp.bfloat16)
            out_copy(flip, spot).start()
        else:
            out_ref[spot] = total.astype(jnp.bfloat16)

    for flip in range(clique):
        if flip:
            mixed_copy(flip).wait_recv()
            for further in flips:
                if further != flip and further - (further & -further) == flip:
                    mixed_copy(further).start()
        multiply(flip, range(given))
    if outer > 1:
        ring.wait_recv()
    for flip in range(clique):
        multiply(flip, range(given, outer))
        for other in lanes:
            piece_copy(flip, other, lane).start()
        if flip:
            settle(flip - 1)
    settle(clique - 1)
    for flip in flips:
        out_copy(flip, flipped(spot, flip)).wait_recv()
    for flip in flips:
        mixed_copy(flip).wait_send()
        out_copy(flip, spot).wait_send()
    for flip in range(clique):
        for other in lanes:
            piece_copy(flip, other, lane).wait_send()
    if outer > 1:
        ring.wait_send()


def ring_weights(held, limit):
    count = lax.axis_size("sp")
    clique = clique_of(count)
    outer = count // clique
    pairs = [(i, (i + clique) % count) for i in range(count)]
    goal = max(outer + limit, 1) if limit < 0 else min(limit, outer)
    held = held[: max(outer - 1, 1)]
    while len(held) < goal:
        held = held + [lax.ppermute(held[-1], "sp", pairs)]
    return held


def flipped(spot, flip):
    bit = 1
    while bit <= flip:
        if flip & bit:
            spot = spot + bit - 2 * bit * lax.rem(spot // bit, 2)
        bit *= 2
    return spot


def project(mixed, weights):
    count = lax.axis_size("sp")
    tps = lax.axis_size("tp")
    clique = clique_of(count)
    outer = count // clique
    rows = mixed.shape[1]
    width = weights[0].shape[2]
    share = rows // tps
    block = (outer, share, width)
    out = pl.pallas_call(
        functools.partial(project_kernel, clique, outer, tps),
        out_shape=jax.ShapeDtypeStruct((clique,) + block, jnp.bfloat16),
        in_specs=[pl.BlockSpec(memory_space=pltpu.VMEM)] * (1 + len(weights)),
        out_specs=pl.BlockSpec(memory_space=pltpu.VMEM),
        scratch_shapes=[
            pltpu.VMEM((clique,) + mixed.shape, jnp.bfloat16),
            pltpu.VMEM((clique, tps) + block, jnp.bfloat16),
            pltpu.VMEM((clique, tps) + block, jnp.bfloat16),
            pltpu.VMEM((clique,) + block, jnp.bfloat16),
            pltpu.SemaphoreType.DMA((2, clique)),
            pltpu.SemaphoreType.DMA((2, clique, tps)),
            pltpu.SemaphoreType.DMA((2, clique)),
            pltpu.VMEM(weights[0].shape, weights[0].dtype),
            pltpu.SemaphoreType.DMA((2,)),
        ],
        compiler_params=pltpu.CompilerParams(collective_id=2, has_side_effects=True),
    )(mixed, *weights)
    return out.transpose(2, 1, 0, 3).reshape(share, outer * clique * width)


def rotate(matrix, offset):
    row_count = matrix.shape[0]
    halfway = HEAD // 2
    heads_here = matrix.shape[1] // HEAD
    spacing = ROTARY_BASE ** (-jnp.arange(halfway, dtype=jnp.float32) * 2.0 / HEAD)
    places = (offset + jnp.arange(row_count, dtype=jnp.int32)).astype(jnp.float32)
    angles = places[:, None] * spacing[None, :]
    cosine = jnp.cos(angles)[:, None, :]
    sine_table = jnp.sin(angles)[:, None, :]
    halves = matrix.astype(jnp.float32).reshape(row_count, heads_here, 2, halfway)
    former = halves[:, :, 0]
    latter = halves[:, :, 1]
    turned = jnp.stack(
        [former * cosine - latter * sine_table, latter * cosine + former * sine_table], axis=2
    )
    return turned.reshape(row_count, heads_here * HEAD).astype(jnp.bfloat16)


def banded(matrix, block_count, kv_here):
    stacked = matrix.reshape(block_count + 2, SPAN, kv_here, HEAD)
    return jnp.concatenate([stacked[:-2], stacked[1:-1], stacked[2:]], axis=1)


def attend(turned_queries, key_band, value_band, absorber_score_vector, offset, seq_total):
    row_count = turned_queries.shape[0]
    block_count = row_count // SPAN
    kv_here = key_band.shape[1] // HEAD
    sharing = turned_queries.shape[1] // HEAD // kv_here
    key_tiles = banded(key_band, block_count, kv_here)
    value_tiles = banded(value_band, block_count, kv_here)
    query_tiles = turned_queries.reshape(block_count, SPAN, kv_here, sharing, HEAD)
    scores = jnp.einsum(
        "bqkgd,bskd->bkgqs", query_tiles, key_tiles, preferred_element_type=jnp.float32
    ) * HEAD ** (-0.5)
    within = jnp.arange(SPAN, dtype=jnp.int32)[:, None]
    across = jnp.arange(3 * SPAN, dtype=jnp.int32)[None, :]
    inside = jnp.abs(across - SPAN - within) <= WINDOW
    places = offset - SPAN + jnp.arange(block_count, dtype=jnp.int32)[:, None] * SPAN + across
    present = (places >= 0) & (places < seq_total)
    allowed = inside[None, :, :] & present[:, None, :]
    scores = jnp.where(allowed[:, None, None, :, :], scores, -jnp.inf)
    sink_rows = absorber_score_vector.reshape(kv_here, sharing)[None, :, :, None, None]
    ceiling = jnp.maximum(jnp.max(scores, axis=-1, keepdims=True), sink_rows)
    weights = jnp.exp(scores - ceiling)
    denominator = jnp.sum(weights, axis=-1, keepdims=True) + jnp.exp(sink_rows - ceiling)
    probabilities = (weights / denominator).astype(jnp.bfloat16)
    attended = jnp.einsum(
        "bkgqs,bskd->bqkgd", probabilities, value_tiles, preferred_element_type=jnp.float32
    )
    return attended.reshape(row_count, turned_queries.shape[1]).astype(jnp.bfloat16)


def convolve(padded, taps_all, row_count):
    summed = jnp.zeros((row_count, padded.shape[1]), jnp.float32)
    for tap_index in range(CONV):
        summed = summed + padded[tap_index : tap_index + row_count].astype(jnp.float32) * taps_all[
            tap_index
        ].astype(jnp.float32)
    return jax.nn.silu(summed).astype(jnp.bfloat16)


def prepare(scan_rows, step_rows, decay_rows, write_rows, read_rows):
    row_count = scan_rows.shape[0]
    block_count = row_count // SPAN
    groups_here = write_rows.shape[1]
    per_group = scan_rows.shape[2]
    step_tiles = step_rows.reshape(block_count, SPAN, groups_here, per_group)
    scaled = (
        scan_rows.astype(jnp.float32).reshape(block_count, SPAN, groups_here, per_group, SSD_HEAD)
        * step_tiles[..., None]
    )
    running = jnp.cumsum(decay_rows.reshape(block_count, SPAN, groups_here, per_group), axis=1)
    write_tiles = write_rows.reshape(block_count, SPAN, groups_here, STATE)
    read_tiles = read_rows.reshape(block_count, SPAN, groups_here, STATE)
    earlier_mask = jnp.arange(SPAN)[:, None] >= jnp.arange(SPAN)[None, :]
    spread = running[:, :, None] - running[:, None, :]
    fading = jnp.exp(jnp.where(earlier_mask[None, :, :, None, None], spread, -jnp.inf))
    affinity = jnp.einsum(
        "blgn,bsgn->blsg", read_tiles, write_tiles, preferred_element_type=jnp.float32
    )
    within_block = jnp.einsum(
        "blsgr,bsgrp->blgrp", affinity[..., None] * fading, scaled
    )
    to_end = jnp.exp(running[:, -1:] - running)
    block_states = jnp.einsum(
        "blgn,blgrp->bgrpn",
        write_tiles.astype(jnp.float32),
        scaled * to_end[..., None],
    )
    totals = running[:, -1]

    def advance(carried, block_item):
        fresh_state, block_total = block_item
        return (carried * jnp.exp(block_total)[..., None, None] + fresh_state, carried)

    final_state, entering = lax.scan(
        advance, jnp.zeros(block_states.shape[1:], jnp.float32), (block_states, totals)
    )
    summary = (jnp.exp(jnp.sum(totals, axis=0)), final_state)
    return ((within_block, entering, running, totals, read_tiles), summary)


def finish(pieces, incoming):
    within_block, entering, running, totals, read_tiles = pieces
    before = jnp.cumsum(totals, axis=0) - totals
    starting = entering + incoming[None] * jnp.exp(before)[..., None, None]
    carried = (
        jnp.einsum(
            "blgn,bgrpn->blgrp",
            read_tiles.astype(jnp.float32),
            starting,
        )
        * jnp.exp(running)[..., None]
    )
    joined = within_block + carried
    return joined.reshape(joined.shape[0] * SPAN, -1)


def local(
    asking_matrix,
    matching_key_matrix,
    carried_value_matrix,
    silu_switch_argument,
    duality_source_matrix,
    storing_direction_matrix,
    fetching_direction_matrix,
    duality_kernel_coefficients,
    storing_kernel_coefficients,
    fetching_kernel_coefficients,
    raw_increment_lengths,
    logarithmic_fading_speeds,
    token_fading_spikes,
    absorber_score_vector,
    cluster_scaling_factor,
    final_mapping_matrix,
):
    row_count = asking_matrix.shape[0]
    offset = lax.axis_index("sp") * row_count
    seq_total = lax.axis_size("sp") * row_count
    weights = ring_weights([final_mapping_matrix], 2)
    turned_queries = rotate(asking_matrix, offset)
    key_value = jnp.concatenate([rotate(matching_key_matrix, offset), carried_value_matrix], axis=1)
    raw_rows = jnp.concatenate(
        [duality_source_matrix, storing_direction_matrix, fetching_direction_matrix], axis=1
    )
    margin = CONV // 2
    pair_rims = padded_2(key_value, (("sp", 0),), WINDOW)
    raw_rims = padded_2(raw_rows, (("sp", 0),), margin)
    filler = jnp.zeros((SPAN - WINDOW, key_value.shape[1]), jnp.bfloat16)
    pair_band = jnp.concatenate([filler, pair_rims, filler], axis=0)
    kv_width = matching_key_matrix.shape[1]
    conved = convolve(
        raw_rims,
        jnp.concatenate(
            [
                duality_kernel_coefficients,
                storing_kernel_coefficients,
                fetching_kernel_coefficients,
            ],
            axis=1,
        ),
        row_count,
    )
    scan_width = duality_source_matrix.shape[1]
    write_width = storing_direction_matrix.shape[1]
    groups_here = write_width // STATE
    per_group = scan_width // SSD_HEAD // groups_here
    scan_rows = conved[:, :scan_width].reshape(row_count, groups_here, per_group, SSD_HEAD)
    write_rows = conved[:, scan_width : scan_width + write_width].reshape(
        row_count, groups_here, STATE
    )
    read_rows = conved[:, scan_width + write_width :].reshape(row_count, groups_here, STATE)
    joint_increment_lengths = jax.nn.softplus(raw_increment_lengths)
    joint_fading_amounts = (
        -jnp.exp(logarithmic_fading_speeds)[:, :, None] * joint_increment_lengths
        + token_fading_spikes
    )
    steps_rows = jnp.transpose(joint_increment_lengths, (0, 2, 1)).reshape(
        2, row_count, groups_here, per_group
    )
    decay_rows = jnp.transpose(joint_fading_amounts, (0, 2, 1)).reshape(
        2, row_count, groups_here, per_group
    )
    ahead_pieces, ahead_summary = prepare(
        scan_rows, steps_rows[0], decay_rows[0], write_rows, read_rows
    )
    back_pieces, back_summary = prepare(
        scan_rows[::-1], steps_rows[1][::-1], decay_rows[1][::-1], write_rows[::-1], read_rows[::-1]
    )
    heads = groups_here * per_group
    incoming, onward = scan_states(
        jnp.stack([ahead_summary[1], back_summary[1]]).reshape(2, heads, SSD_HEAD, STATE),
        jnp.stack([ahead_summary[0], back_summary[0]]).reshape(2, heads),
        weights[-1],
    )
    weights = ring_weights(weights + [onward], -1)
    incoming = incoming.reshape(2, groups_here, per_group, SSD_HEAD, STATE)
    turned_queries, incoming = lax.optimization_barrier((turned_queries, incoming))
    attended = attend(
        turned_queries,
        pair_band[:, :kv_width],
        pair_band[:, kv_width:],
        absorber_score_vector,
        offset,
        seq_total,
    )
    both_ways = finish(ahead_pieces, incoming[0].astype(jnp.float32)) + finish(
        back_pieces, incoming[1].astype(jnp.float32)
    )[::-1]
    gated_rows = both_ways * jax.nn.silu(silu_switch_argument.astype(jnp.float32))
    grouped = gated_rows.reshape(row_count, groups_here, -1)
    grouped = grouped * lax.rsqrt(jnp.mean(grouped * grouped, axis=-1, keepdims=True) + EPSILON)
    normed = (grouped.reshape(row_count, scan_width) * cluster_scaling_factor).astype(jnp.bfloat16)
    return project(jnp.stack([attended, normed]), weights)


def solution(mesh):
    in_specs = (
        P("sp", "tp"),
        P("sp", "tp"),
        P("sp", "tp"),
        P("sp", "tp"),
        P("sp", "tp"),
        P("sp", "tp"),
        P("sp", "tp"),
        P(None, "tp"),
        P(None, "tp"),
        P(None, "tp"),
        P(None, "tp", "sp"),
        P(None, "tp"),
        P(None, "tp", "sp"),
        P("tp"),
        P("tp"),
        P(None, "tp", "sp"),
    )
    out_specs = P(("sp", "tp"), None)
    return jax.shard_map(local, mesh=mesh, in_specs=in_specs, out_specs=out_specs, check_vma=False)
```
